32 devices in a mesh: ep: 8 (over z, x), tp: 4 (over y, core).
Axes of the slice: x: 2, y: 2, z: 4, core: 2. Of those that a mesh axis runs over, the one named last changes fastest.
Arguments:
- conv_value: bfloat16 [1024, 4096], P('tp', 'ep'), may hold values from -6 to 6
- conv_gate: bfloat16 [1024, 4096], P('tp', 'ep'), may hold values from -8 to 8
- conv_kernel: bfloat16 [31, 1024], P(None, 'tp'), may hold values from -1 to 1
- norm_gain: float32 [1024], replicated, may hold values from 0.1 to 1.9
- norm_shift: float32 [1024], replicated, may hold values from -3 to 3
- out_weight: bfloat16 [1024, 4096], P(None, 'tp'), may hold values from -0.1875 to 0.1875
- expert_input: bfloat16 [1024, 4096], P('ep'), may hold values from -6 to 6
- expert_ids: int32 [1024, 2], P('ep'), may hold values from 0 to 7, as said below
- pair_logits: float32 [1024, 2], P('ep'), may hold values from -6 to 6
- group_prob: float32 [1024], P('ep'), may hold values from 0.3 to 1
- expert_gate: bfloat16 [8, 4096, 2048], P('ep', None, 'tp'), may hold values from -0.09375 to 0.09375
- expert_up: bfloat16 [8, 4096, 2048], P('ep', None, 'tp'), may hold values from -0.09375 to 0.09375
- expert_down: bfloat16 [8, 2048, 4096], P('ep', None, 'tp'), may hold values from -0.125 to 0.125
Outputs:
- mixer_out: bfloat16 [4096, 4096], P('ep', 'tp')
- expert_out: bfloat16 [1024, 4096], P('ep', 'tp')
The draws below stay inside these ranges and needn't reach their ends.
Inputs may be any that keep to these rules, and one draw needn't show every extreme that they name: `expert_ids`: the two experts of a token differ and lie in one group, ids g * 2 to (g + 1) * 2 - 1 for some g. The 128 tokens of one index of ep name every expert exactly 32 times.
All inputs are finite; a program needn't handle non-finite values.
Results may differ from the reference program's by a relative error of at most 0.0064.
Values may be sent and summed in bfloat16 or wider, within the bound.
A program may use at most 64 MiB of HBM per device.

```python
import jax
import jax.numpy as jnp
from jax import lax

D = 4096
CONV_CH = 1024
KERNEL = 31
EXPERT_FF = 2048
GROUPS = 4
B_DEV = 128
EXPERTS = 8
TOK_A = 4096
TOK_B = 1024


def draw_expert_ids(key, part):
    group_size = EXPERTS // GROUPS
    blocks = TOK_B // B_DEV

    def one_block(block_key):
        key_order, key_offset, key_stride = jax.random.split(block_key, 3)
        order = jax.random.permutation(key_order, B_DEV)
        places = jnp.arange(B_DEV, dtype=jnp.int32)
        group = places % GROUPS
        ordinal = places // GROUPS
        offsets = jax.random.randint(key_offset, (GROUPS,), 0, group_size)
        strides = jax.random.randint(key_stride, (GROUPS,), 0, group_size - 1)
        first = (ordinal + offsets[group]) % group_size
        second = (first + 1 + strides[group]) % group_size
        chosen = jnp.stack([group * group_size + first, group * group_size + second], axis=1).astype(jnp.int32)
        return jnp.zeros((B_DEV, 2), jnp.int32).at[order].set(chosen)
    block_keys = jax.random.split(jax.random.fold_in(key, 17), blocks)
    return jax.vmap(one_block)(block_keys).reshape(TOK_B, 2).astype(jnp.int32)


def block_levels(stream_key, dims, shards, low, largest):
    level, own = 1.0, jax.random.fold_in(stream_key, 6)
    for dim, shards_of in shards:
        steps = jnp.exp(jax.random.uniform(jax.random.fold_in(own, dim), (shards_of,), jnp.float32, low / len(shards), largest / len(shards)))
        level = level * jnp.repeat(steps, dims[dim] // shards_of).reshape([-1 if axis == dim else 1 for axis in range(len(dims))])
    return level


def gaussian(stream_key, dims, scale, bound, cuts=(), held_as=jnp.bfloat16):
    factor_of = block_levels(stream_key, dims, cuts, -0.22, 0.18) if cuts else 1.0
    drawn = jax.random.normal(stream_key, dims, jnp.float32) * scale * factor_of
    return jnp.minimum(jnp.maximum(drawn, -bound), bound).astype(held_as)


def setup_inputs(seed: int = 0) -> dict:
    key_of = jax.random.split(jax.random.key(seed), 14)
    return {
        "conv_value": gaussian(key_of[0], (CONV_CH, TOK_A), 1.0, 6.0, ((0, 4), (1, 8))),
        "conv_gate": gaussian(key_of[1], (CONV_CH, TOK_A), 1.5, 8.0, ((0, 4), (1, 8))),
        "conv_kernel": gaussian(key_of[2], (KERNEL, CONV_CH), KERNEL ** -0.5, 1.0, ((1, 4),)),
        "norm_gain": jnp.clip(1.0 + 0.18 * jax.random.normal(key_of[3], (CONV_CH,), jnp.float32), 0.1, 1.9),
        "norm_shift": gaussian(key_of[4], (CONV_CH,), 0.5, 3.0, (), jnp.float32),
        "out_weight": gaussian(key_of[5], (CONV_CH, D), CONV_CH ** -0.5, 0.1875, ((1, 4),)),
        "expert_input": gaussian(key_of[6], (TOK_B, D), 1.0, 6.0, ((0, 8),)),
        "expert_ids": draw_expert_ids(jax.random.fold_in(key_of[13], 71), 0),
        "pair_logits": gaussian(key_of[8], (TOK_B, 2), 1.5, 6.0, ((0, 8),), jnp.float32),
        "group_prob": jnp.clip(0.3 + 0.7 * jax.random.uniform(key_of[9], (TOK_B,), jnp.float32) ** block_levels(key_of[9], (TOK_B,), ((0, 8),), -0.2, 0.2), 0.3, 1.0),
        "expert_gate": gaussian(key_of[10], (EXPERTS, D, EXPERT_FF), D ** -0.5, 0.09375, ((0, 8), (2, 4))),
        "expert_up": gaussian(key_of[11], (EXPERTS, D, EXPERT_FF), D ** -0.5, 0.09375, ((0, 8), (2, 4))),
        "expert_down": gaussian(key_of[12], (EXPERTS, EXPERT_FF, D), EXPERT_FF ** -0.5, 0.125, ((0, 8), (2, 4))),
    }


def norm_swish(conv_out, norm_gain, norm_shift):
    values = conv_out.astype(jnp.float32)
    center = lax.optimization_barrier(jnp.mean(values, axis=0, keepdims=True))
    spread = lax.optimization_barrier(jnp.mean(jnp.square(values - center), axis=0, keepdims=True))
    normed = (values - center) * lax.rsqrt(spread + 1e-05) * norm_gain[:, None] + norm_shift[:, None]
    return jax.nn.silu(normed).astype(jnp.bfloat16)

def route_weights(pair_logits, group_prob):
    share = jax.nn.sigmoid(pair_logits[:, 0] - pair_logits[:, 1])
    return jnp.stack([share, 1.0 - share], axis=1) * group_prob[:, None]

def reference(conv_value, conv_gate, conv_kernel, norm_gain, norm_shift, out_weight, expert_input, expert_ids, pair_logits, group_prob, expert_gate, expert_up, expert_down):
    gated = (conv_value.astype(jnp.float32) * jax.nn.sigmoid(conv_gate.astype(jnp.float32))).astype(jnp.bfloat16)
    reach = (KERNEL - 1) // 2
    length = gated.shape[1]
    padded = jnp.pad(gated.astype(jnp.float32), ((0, 0), (reach, reach)))
    kernel_f = conv_kernel.astype(jnp.float32)
    summed = jnp.zeros(gated.shape, jnp.float32)
    for offset in range(KERNEL):
        summed = summed + kernel_f[offset][:, None] * padded[:, offset:offset + length]
    conv_out = summed.astype(jnp.bfloat16)
    swished = norm_swish(conv_out, norm_gain, norm_shift)
    mixer_out = lax.dot_general(swished, out_weight, (((0,), (0,)), ((), ())), preferred_element_type=jnp.float32).astype(jnp.bfloat16)
    weights = route_weights(pair_logits, group_prob)
    flat = expert_ids.reshape(-1).astype(jnp.int32)
    order = jnp.argsort(flat, stable=True).astype(jnp.int32)
    experts_all = expert_gate.shape[0]
    per_expert = flat.shape[0] // experts_all
    rows = (order // 2).astype(jnp.int32).reshape(experts_all, per_expert)

    def one_expert(packed):
        rows_here, gate_w, up_w, down_w = packed
        block = expert_input[rows_here]
        gate_val = jnp.dot(block, gate_w, preferred_element_type=jnp.float32)
        up_val = jnp.dot(block, up_w, preferred_element_type=jnp.float32)
        hidden = (jax.nn.silu(gate_val) * up_val).astype(jnp.bfloat16)
        return jnp.dot(hidden, down_w, preferred_element_type=jnp.float32).astype(jnp.bfloat16)
    results = lax.map(one_expert, (rows, expert_gate, expert_up, expert_down))
    width = expert_input.shape[1]
    copies = jnp.zeros((flat.shape[0], width), jnp.bfloat16).at[order].set(results.reshape(-1, width))
    copies = copies.reshape(-1, 2, width).astype(jnp.float32)
    expert_out = lax.optimization_barrier(jnp.sum(copies * weights[:, :, None], axis=1)).astype(jnp.bfloat16)
    return (mixer_out, expert_out)
```

```python
import functools

import jax
import jax.numpy as jnp
from jax import lax
from jax.experimental import pallas as pl
from jax.experimental.pallas import tpu as pltpu
from jax.sharding import PartitionSpec as P

MESH = pl.DeviceIdType.MESH
CORES = 2
F32, BF16 = jnp.float32, jnp.bfloat16


def tiles(size, most):
    tile = min(size, most)
    return tile, size // tile


def kernel(
    experts,
    parts,
    value_hbm,
    gate_hbm,
    input_hbm,
    wgate_hbm,
    wup_hbm,
    wdown_hbm,
    wout_hbm,
    taps_ref,
    gain_ref,
    shift_ref,
    ids_ref,
    logits_ref,
    prob_ref,
    mixer_hbm,
    expert_hbm,
    value,
    gate,
    tokens,
    wgate,
    wup,
    wdown,
    wout,
    send_rows,
    arrived,
    gate_sum,
    up_sum,
    hidden,
    down_sum,
    result,
    returned,
    padded,
    edges,
    halo,
    conv,
    swished,
    mixer,
    combined,
    load_sem,
    out_sem,
    self_sem,
    disp_send,
    disp_recv,
    fwd_send,
    fwd_recv,
    hal_send,
    hal_recv,
    conv_send,
    conv_recv,
    hid_send,
    hid_recv,
    ret_send,
    ret_recv,
):
    me = lax.axis_index("ep")
    tp = lax.axis_index("tp")
    chips = parts // CORES
    chip, core = lax.div(tp, CORES), lax.rem(tp, CORES)
    other = 1 - core
    sibling = chip * CORES + other
    slots = send_rows.shape[1]
    half = send_rows.shape[2]
    rows = experts * slots
    length, channels = conv.shape[1], conv.shape[2]
    edge = halo.shape[1]
    reach = (taps_ref.shape[0] - 1) // 2

    def remote(src, dst, ssem, rsem, ep=None, part=None):
        target = (me if ep is None else ep, tp if part is None else part)
        return pltpu.make_async_remote_copy(
            src_ref=src, dst_ref=dst, send_sem=ssem, recv_sem=rsem, device_id=target, device_id_type=MESH
        )

    def ahead(k):
        return lax.rem(me + k, experts)

    def behind(k):
        return lax.rem(me + experts - k, experts)

    def chip_ahead(k):
        return lax.rem(chip + k, chips) * CORES + core

    def chip_behind(k):
        return lax.rem(chip + chips - k, chips) * CORES + core

    barrier = pltpu.get_barrier_semaphore()

    @pl.loop(1, experts)
    def _(k):
        pl.semaphore_signal(barrier, inc=1, device_id=(ahead(k), tp), device_id_type=MESH)

    @pl.loop(1, chips)
    def _(k):
        pl.semaphore_signal(barrier, inc=1, device_id=(me, chip_ahead(k)), device_id_type=MESH)

    pl.semaphore_signal(barrier, inc=1, device_id=(me, sibling), device_id_type=MESH)

    columns = pl.ds(pl.multiple_of(core * half, half), half)
    loads = [
        pltpu.make_async_copy(src, dst, load_sem.at[i])
        for i, (src, dst) in enumerate(
            [
                (input_hbm.at[:, columns], tokens),
                (value_hbm, value),
                (gate_hbm, gate),
                (wgate_hbm.at[0], wgate),
                (wup_hbm.at[0], wup),
                (wout_hbm, wout),
                (wdown_hbm.at[0], wdown),
            ]
        )
    ]
    for load in loads:
        load.start()

    count = ids_ref.shape[1]
    first, second = ids_ref[0:1, :], ids_ref[1:2, :]
    expert_of = lax.broadcasted_iota(jnp.int32, (experts, count), 0)
    is_first, is_second = expert_of == first, expert_of == second
    chosen = jnp.where(is_first | is_second, 1.0, 0.0).astype(F32)
    earlier = lax.broadcasted_iota(jnp.int32, (count, count), 0) < lax.broadcasted_iota(
        jnp.int32, (count, count), 1
    )
    rank = jnp.dot(
        chosen.astype(BF16), jnp.where(earlier, 1.0, 0.0).astype(BF16), preferred_element_type=F32
    )
    rank = jnp.where(chosen > 0, rank, -1.0)
    ordinal = lax.broadcasted_iota(jnp.int32, (experts, slots, count), 1).astype(F32)
    place3 = jnp.broadcast_to(rank[:, None, :], (experts, slots, count)) == ordinal
    place = jnp.where(place3, 1.0, 0.0).astype(F32).reshape(rows, count)

    loads[0].wait()
    tile, steps = tiles(half, 512)
    for i in range(steps):
        span = slice(i * tile, (i + 1) * tile)
        picked = jnp.dot(place.astype(BF16), tokens[:, span], preferred_element_type=F32)
        send_rows[:, :, span] = picked.reshape(experts, slots, tile).astype(BF16)

    pl.semaphore_wait(barrier, experts - 1 + chips)

    def dispatch(k):
        return remote(
            send_rows.at[ahead(k)], arrived.at[core, me], disp_send.at[k], disp_recv.at[k], ep=ahead(k)
        )

    def forward(k, src):
        return remote(
            src, arrived.at[core, behind(k)], fwd_send.at[k], fwd_recv.at[k], part=sibling
        )

    @pl.loop(1, experts)
    def _(k):
        dispatch(k).start()

    keep = pltpu.make_async_copy(send_rows.at[me], arrived.at[core, me], self_sem.at[0])
    keep.start()
    forward(0, send_rows.at[me]).start()

    loads[1].wait()
    loads[2].wait()
    gated = (value[...].astype(F32) * jax.nn.sigmoid(gate[...].astype(F32))).astype(BF16)
    padded[edge : edge + length, :] = jnp.transpose(gated.astype(F32), (1, 0))
    edges[0] = padded[edge : 2 * edge, :].astype(BF16)
    edges[1] = padded[length : length + edge, :].astype(BF16)
    to_left = remote(edges.at[0], halo.at[1], hal_send.at[0], hal_recv.at[0], ep=behind(1))
    to_right = remote(edges.at[1], halo.at[0], hal_send.at[1], hal_recv.at[1], ep=ahead(1))
    to_left.start()
    to_right.start()
    taps = taps_ref[...].astype(F32)
    chunk, chunks = tiles(length, 64)

    def convolve(i):
        total = jnp.zeros((chunk, channels), F32)
        for j in range(taps.shape[0]):
            start = i * chunk + j + edge - reach
            total = total + taps[j : j + 1, :] * padded[start : start + chunk, :]
        conv[tp, i * chunk : (i + 1) * chunk, :] = total.astype(BF16)

    for i in range(1, chunks - 1):
        convolve(i)
    to_left.wait()
    to_right.wait()
    padded[0:edge, :] = jnp.where(me == 0, 0.0, halo[0].astype(F32))
    padded[edge + length : 2 * edge + length, :] = jnp.where(
        me == experts - 1, 0.0, halo[1].astype(F32)
    )
    convolve(0)
    convolve(chunks - 1)

    def gather(buffer, ssem, rsem):
        def across(k):
            return remote(buffer.at[tp], buffer.at[tp], ssem.at[k], rsem.at[k], part=chip_ahead(k))

        def beside(k):
            block = chip_behind(k)
            return remote(
                buffer.at[block], buffer.at[block], ssem.at[chips + k], rsem.at[chips + k], part=sibling
            )

        return across, beside

    conv_across, conv_beside = gather(conv, conv_send, conv_recv)

    @pl.loop(1, chips)
    def _(k):
        conv_across(k).start()

    conv_beside(0).start()

    @pl.loop(1, experts)
    def _(k):
        dispatch(k).wait_recv()
        forward(k, arrived.at[core, behind(k)]).start()

    keep.wait()
    loads[3].wait()
    loads[4].wait()
    units = gate_sum.shape[1]
    tile, steps = tiles(units, 256)

    def side(which):
        block = arrived[which]
        if slots % 16:
            return block.astype(F32).reshape(rows, half).astype(BF16)
        return block.reshape(rows, half)

    def depth(which):
        return pl.ds(pl.multiple_of(which * half, half), half)

    for i in range(steps):
        span = slice(i * tile, (i + 1) * tile)
        gate_sum[:, span] = jnp.dot(side(core), wgate[depth(core), span], preferred_element_type=F32)
        up_sum[:, span] = jnp.dot(side(core), wup[depth(core), span], preferred_element_type=F32)

    @pl.loop(0, experts)
    def _(k):
        forward(k, send_rows.at[me]).wait_recv()

    for i in range(steps):
        span = slice(i * tile, (i + 1) * tile)
        gate_val = gate_sum[:, span] + jnp.dot(
            side(other), wgate[depth(other), span], preferred_element_type=F32
        )
        up_val = up_sum[:, span] + jnp.dot(
            side(other), wup[depth(other), span], preferred_element_type=F32
        )
        hidden[tp, :, span] = (jax.nn.silu(gate_val) * up_val).astype(BF16)

    hid_across, hid_beside = gather(hidden, hid_send, hid_recv)

    @pl.loop(1, chips)
    def _(k):
        hid_across(k).start()

    hid_beside(0).start()

    @pl.loop(1, chips)
    def _(k):
        conv_across(k).wait_recv()
        conv_beside(k).start()

    @pl.loop(0, chips)
    def _(k):
        conv_beside(k).wait_recv()

    width = parts * channels
    chunk, chunks = tiles(length, 64)

    @pl.loop(0, chunks)
    def _(i):
        span = pl.ds(pl.multiple_of(i * chunk, chunk), chunk)
        blocks = [conv[b, span, :].astype(F32) for b in range(parts)]
        center = sum(jnp.sum(block, axis=1, keepdims=True) for block in blocks) / width
        blocks = [block - center for block in blocks]
        spread = sum(jnp.sum(block * block, axis=1, keepdims=True) for block in blocks) / width
        scale = lax.rsqrt(spread + 1e-05)
        for b in range(parts):
            lanes = slice(b * channels, (b + 1) * channels)
            normed = blocks[b] * scale * gain_ref[:, lanes] + shift_ref[:, lanes]
            swished[b, span, :] = jax.nn.silu(normed).astype(BF16)

    loads[6].wait()
    wide = down_sum.shape[1]
    tile, steps = tiles(wide, 256)

    def down(block, begin):
        deep = pl.ds(pl.multiple_of(block * units, units), units)

        @pl.loop(0, steps)
        def _(i):
            span = pl.ds(pl.multiple_of(i * tile, tile), tile)
            product = jnp.dot(hidden[block], wdown[deep, span], preferred_element_type=F32)
            down_sum[:, span] = product if begin else down_sum[:, span] + product

    down(tp, True)
    hid_beside(0).wait_recv()
    down(sibling, False)

    @pl.loop(1, chips)
    def _(k):
        hid_across(k).wait_recv()
        hid_beside(k).start()
        down(chip_behind(k), False)
        hid_beside(k).wait_recv()
        down(chip_behind(k) + other - core, False)

    result[...] = down_sum[...].reshape(experts, slots, wide).astype(BF16)

    def give_back(k):
        return remote(result.at[ahead(k)], returned.at[me], ret_send.at[k], ret_recv.at[k], ep=ahead(k))

    @pl.loop(1, experts)
    def _(k):
        give_back(k).start()

    own = pltpu.make_async_copy(result.at[me], returned.at[me], self_sem.at[1])
    own.start()

    loads[5].wait()
    tile, steps = tiles(mixer.shape[1], 256)

    @pl.loop(0, steps)
    def _(i):
        span = pl.ds(pl.multiple_of(i * tile, tile), tile)
        total = jnp.zeros((length, tile), F32)
        for b in range(parts):
            total = total + jnp.dot(
                swished[b], wout[b * channels : (b + 1) * channels, span], preferred_element_type=F32
            )
        mixer[:, span] = total.astype(BF16)

    put_mixer = pltpu.make_async_copy(mixer, mixer_hbm, out_sem.at[0])
    put_mixer.start()

    share = jax.nn.sigmoid(logits_ref[0:1, :] - logits_ref[1:2, :])
    weight = jnp.where(is_first, share * prob_ref[...], 0.0) + jnp.where(
        is_second, (1.0 - share) * prob_ref[...], 0.0
    )
    weights = jnp.where(
        place3, jnp.broadcast_to(weight[:, None, :], (experts, slots, count)), 0.0
    ).reshape(rows, count)
    weights = jnp.transpose(weights, (1, 0))
    high = weights.astype(BF16)
    rest = weights - high.astype(F32)
    middle = rest.astype(BF16)
    low = (rest - middle.astype(F32)).astype(BF16)

    own.wait()

    @pl.loop(1, experts)
    def _(k):
        give_back(k).wait_recv()

    tile, steps = tiles(wide, 512)
    for i in range(steps):
        span = slice(i * tile, (i + 1) * tile)
        block = returned[:, :, span]
        if slots % 16:
            block = block.astype(F32).reshape(rows, tile).astype(BF16)
        else:
            block = block.reshape(rows, tile)
        total = jnp.dot(low, block, preferred_element_type=F32)
        total = total + jnp.dot(middle, block, preferred_element_type=F32)
        total = total + jnp.dot(high, block, preferred_element_type=F32)
        combined[:, span] = total.astype(BF16)

    put_expert = pltpu.make_async_copy(combined, expert_hbm, out_sem.at[1])
    put_expert.start()

    @pl.loop(1, experts)
    def _(k):
        dispatch(k).wait_send()
        give_back(k).wait_send()

    @pl.loop(0, experts)
    def _(k):
        forward(k, send_rows.at[me]).wait_send()

    @pl.loop(1, chips)
    def _(k):
        conv_across(k).wait_send()
        hid_across(k).wait_send()

    @pl.loop(0, chips)
    def _(k):
        conv_beside(k).wait_send()
        hid_beside(k).wait_send()

    put_mixer.wait()
    put_expert.wait()


def local(
    experts,
    parts,
    conv_value,
    conv_gate,
    conv_kernel,
    norm_gain,
    norm_shift,
    out_weight,
    expert_input,
    expert_ids,
    pair_logits,
    group_prob,
    expert_gate,
    expert_up,
    expert_down,
):
    channels, length = conv_value.shape
    count, model = expert_input.shape
    slots = 2 * count // experts
    rows = experts * slots
    half = model // CORES
    units, wide = expert_gate.shape[2], expert_down.shape[2]
    out_width = out_weight.shape[1]
    chips = parts // CORES
    edge = -(-((conv_kernel.shape[0] - 1) // 2) // 16) * 16
    anywhere = pl.BlockSpec(memory_space=pl.ANY)
    near = pl.BlockSpec(memory_space=pltpu.VMEM)
    dma = pltpu.SemaphoreType.DMA
    return pl.pallas_call(
        functools.partial(kernel, experts, parts),
        out_shape=(
            jax.ShapeDtypeStruct((length, out_width), BF16),
            jax.ShapeDtypeStruct((count, wide), BF16),
        ),
        in_specs=[anywhere] * 7 + [near] * 6,
        out_specs=(anywhere, anywhere),
        scratch_shapes=[
            pltpu.VMEM((channels, length), BF16),
            pltpu.VMEM((channels, length), BF16),
            pltpu.VMEM((count, half), BF16),
            pltpu.VMEM((model, units), BF16),
            pltpu.VMEM((model, units), BF16),
            pltpu.VMEM(expert_down.shape[1:], BF16),
            pltpu.VMEM(out_weight.shape, BF16),
            pltpu.VMEM((experts, slots, half), BF16),
            pltpu.VMEM((CORES, experts, slots, half), BF16),
            pltpu.VMEM((rows, units), F32),
            pltpu.VMEM((rows, units), F32),
            pltpu.VMEM((parts, rows, units), BF16),
            pltpu.VMEM((rows, wide), F32),
            pltpu.VMEM((experts, slots, wide), BF16),
            pltpu.VMEM((experts, slots, wide), BF16),
            pltpu.VMEM((length + 2 * edge, channels), F32),
            pltpu.VMEM((2, edge, channels), BF16),
            pltpu.VMEM((2, edge, channels), BF16),
            pltpu.VMEM((parts, length, channels), BF16),
            pltpu.VMEM((parts, length, channels), BF16),
            pltpu.VMEM((length, out_width), BF16),
            pltpu.VMEM((count, wide), BF16),
            dma((7,)),
            dma((2,)),
            dma((2,)),
            dma((experts,)),
            dma((experts,)),
            dma((experts,)),
            dma((experts,)),
            dma((2,)),
            dma((2,)),
            dma((2 * chips,)),
            dma((2 * chips,)),
            dma((2 * chips,)),
            dma((2 * chips,)),
            dma((experts,)),
            dma((experts,)),
        ],
        compiler_params=pltpu.CompilerParams(
            collective_id=0, has_side_effects=True, vmem_limit_bytes=60 * 1024 * 1024
        ),
        name="block",
    )(
        conv_value,
        conv_gate,
        expert_input,
        expert_gate,
        expert_up,
        expert_down,
        out_weight,
        conv_kernel,
        norm_gain[None, :],
        norm_shift[None, :],
        expert_ids.T,
        pair_logits.T,
        group_prob[None, :],
    )


def solution(mesh):
    placed = (
        P("tp", "ep"),
        P("tp", "ep"),
        P(None, "tp"),
        P(),
        P(),
        P(None, "tp"),
        P("ep", None),
        P("ep", None),
        P("ep", None),
        P("ep"),
        P("ep", None, "tp"),
        P("ep", None, "tp"),
        P("ep", None, "tp"),
    )
    return jax.shard_map(
        functools.partial(local, mesh.shape["ep"], mesh.shape["tp"]),
        mesh=mesh,
        in_specs=placed,
        out_specs=(P("ep", "tp"), P("ep", "tp")),
        check_vma=False,
    )
```

```python
import functools

import jax
import jax.numpy as jnp
from jax import lax
from jax.experimental import pallas as pl
from jax.experimental.pallas import tpu as pltpu
from jax.sharding import PartitionSpec as P

MESH = pl.DeviceIdType.MESH
CORES = 2
F32, BF16 = jnp.float32, jnp.bfloat16


def tiles(size, most):
    tile = min(size, most)
    return tile, size // tile


def kernel(
    experts,
    parts,
    value_hbm,
    gate_hbm,
    input_hbm,
    wgate_hbm,
    wup_hbm,
    wdown_hbm,
    wout_hbm,
    taps_ref,
    gain_ref,
    shift_ref,
    ids_ref,
    logits_ref,
    prob_ref,
    mixer_hbm,
    expert_hbm,
    value,
    gate,
    tokens,
    wgate,
    wup,
    wdown,
    wout,
    send_rows,
    arrived,
    hidden,
    down_sum,
    result,
    returned,
    padded,
    edges,
    halo,
    conv,
    swished,
    mixer,
    combined,
    load_sem,
    out_sem,
    self_sem,
    disp_send,
    disp_recv,
    side_send,
    side_recv,
    far_send,
    far_recv,
    hal_send,
    hal_recv,
    conv_send,
    conv_recv,
    hid_send,
    hid_recv,
    ret_send,
    ret_recv,
):
    me = lax.axis_index("ep")
    tp = lax.axis_index("tp")
    chips = parts // CORES
    chip, core = lax.div(tp, CORES), lax.rem(tp, CORES)
    other = 1 - core
    sibling = chip * CORES + other
    slots = send_rows.shape[1]
    part_width = send_rows.shape[2]
    near = experts // 2
    base = lax.div(me, near) * near
    place_in = lax.rem(me, near)
    rows = experts * slots
    length, channels = conv.shape[1], conv.shape[2]
    edge = halo.shape[1]
    reach = (taps_ref.shape[0] - 1) // 2

    def remote(src, dst, ssem, rsem, ep=None, part=None):
        target = (me if ep is None else ep, tp if part is None else part)
        return pltpu.make_async_remote_copy(
            src_ref=src, dst_ref=dst, send_sem=ssem, recv_sem=rsem, device_id=target, device_id_type=MESH
        )

    def ahead(k):
        return lax.rem(me + k, experts)

    def behind(k):
        return lax.rem(me + experts - k, experts)

    def chip_ahead(k):
        return lax.rem(chip + k, chips) * CORES + core

    def chip_behind(k):
        return lax.rem(chip + chips - k, chips) * CORES + core

    barrier = pltpu.get_barrier_semaphore()

    @pl.loop(1, experts)
    def _(k):
        pl.semaphore_signal(barrier, inc=1, device_id=(ahead(k), tp), device_id_type=MESH)

    @pl.loop(1, chips)
    def _(k):
        pl.semaphore_signal(barrier, inc=1, device_id=(me, chip_ahead(k)), device_id_type=MESH)

    pl.semaphore_signal(barrier, inc=1, device_id=(me, sibling), device_id_type=MESH)

    columns = pl.ds(pl.multiple_of(tp * part_width, part_width), part_width)
    loads = [
        pltpu.make_async_copy(src, dst, load_sem.at[i])
        for i, (src, dst) in enumerate(
            [
                (input_hbm.at[:, columns], tokens),
                (value_hbm, value),
                (gate_hbm, gate),
                (wgate_hbm.at[0], wgate),
                (wup_hbm.at[0], wup),
                (wout_hbm, wout),
                (wdown_hbm.at[0], wdown),
            ]
        )
    ]
    for load in loads:
        load.start()

    count = ids_ref.shape[1]
    first, second = ids_ref[0:1, :], ids_ref[1:2, :]
    expert_of = lax.broadcasted_iota(jnp.int32, (experts, count), 0)
    is_first, is_second = expert_of == first, expert_of == second
    chosen = jnp.where(is_first | is_second, 1.0, 0.0).astype(F32)
    earlier = lax.broadcasted_iota(jnp.int32, (count, count), 0) < lax.broadcasted_iota(
        jnp.int32, (count, count), 1
    )
    rank = jnp.dot(
        chosen.astype(BF16), jnp.where(earlier, 1.0, 0.0).astype(BF16), preferred_element_type=F32
    )
    rank = jnp.where(chosen > 0, rank, -1.0)
    ordinal = lax.broadcasted_iota(jnp.int32, (experts, slots, count), 1).astype(F32)
    place3 = jnp.broadcast_to(rank[:, None, :], (experts, slots, count)) == ordinal
    place = jnp.where(place3, 1.0, 0.0).astype(F32).reshape(rows, count)

    loads[0].wait()
    tile, steps = tiles(part_width, 512)
    for i in range(steps):
        span = slice(i * tile, (i + 1) * tile)
        picked = jnp.dot(place.astype(BF16), tokens[:, span], preferred_element_type=F32)
        send_rows[:, :, span] = picked.reshape(experts, slots, tile).astype(BF16)

    pl.semaphore_wait(barrier, experts - 1 + chips)

    def partner(j, sign, crosses):
        start = near - base if crosses else base
        return start + lax.rem(place_in + near + sign * (j - near if crosses else j), near)

    def dispatch(j, crosses):
        to = partner(j, 1, crosses)
        return remote(send_rows.at[to], arrived.at[tp, me], disp_send.at[j], disp_recv.at[j], ep=to)

    def row_block(j, k, crosses):
        return arrived.at[chip_behind(k), partner(j, -1, crosses)]

    def to_side(j, k, crosses, src=None):
        block = row_block(j, k, crosses)
        at = k * experts + j
        return remote(
            block if src is None else src, block, side_send.at[at], side_recv.at[at], part=sibling
        )

    def to_far(j, k, crosses, src=None):
        block = row_block(j, 0, crosses)
        at = k * experts + j
        return remote(
            block if src is None else src, block, far_send.at[at], far_recv.at[at], part=chip_ahead(k)
        )

    def spread(j, crosses, src=None):
        @pl.loop(1, chips)
        def _(k):
            to_far(j, k, crosses, src).start()

        to_side(j, 0, crosses, src).start()

    for crosses in (False, True):

        @pl.loop(near if crosses else 1, experts if crosses else near)
        def _(j):
            dispatch(j, crosses).start()

    keep = pltpu.make_async_copy(send_rows.at[me], arrived.at[tp, me], self_sem.at[0])
    keep.start()
    spread(0, False, send_rows.at[me])

    loads[1].wait()
    loads[2].wait()
    gated = (value[...].astype(F32) * jax.nn.sigmoid(gate[...].astype(F32))).astype(BF16)
    padded[edge : edge + length, :] = jnp.transpose(gated.astype(F32), (1, 0))
    edges[0] = padded[edge : 2 * edge, :].astype(BF16)
    edges[1] = padded[length : length + edge, :].astype(BF16)
    to_left = remote(edges.at[0], halo.at[1], hal_send.at[0], hal_recv.at[0], ep=behind(1))
    to_right = remote(edges.at[1], halo.at[0], hal_send.at[1], hal_recv.at[1], ep=ahead(1))
    to_left.start()
    to_right.start()
    taps = taps_ref[...].astype(F32)
    chunk, chunks = tiles(length, 64)

    def convolve(i):
        total = jnp.zeros((chunk, channels), F32)
        for j in range(taps.shape[0]):
            start = i * chunk + j + edge - reach
            total = total + taps[j : j + 1, :] * padded[start : start + chunk, :]
        conv[tp, i * chunk : (i + 1) * chunk, :] = total.astype(BF16)

    early = chunks // 2
    for i in range(1, early):
        convolve(i)
    to_left.wait()
    to_right.wait()
    padded[0:edge, :] = jnp.where(me == 0, 0.0, halo[0].astype(F32))
    padded[edge + length : 2 * edge + length, :] = jnp.where(
        me == experts - 1, 0.0, halo[1].astype(F32)
    )

    def gather(block_of, ssem, rsem):
        def across(k):
            block = block_of(tp)
            return remote(block, block, ssem(k), rsem(k), part=chip_ahead(k))

        def beside(k):
            block = block_of(chip_behind(k))
            return remote(block, block, ssem(chips + k), rsem(chips + k), part=sibling)

        def begin():
            @pl.loop(1, chips)
            def _(k):
                across(k).start()

            beside(0).start()

        return across, beside, begin

    conv_across, conv_beside, conv_begin = gather(
        lambda b: conv.at[b], lambda k: conv_send.at[k], lambda k: conv_recv.at[k]
    )

    units = hidden.shape[3]
    tile, steps = tiles(units, 256)
    group_rows = near * slots

    def join(block):
        if slots % 16:
            return block.astype(F32).reshape(group_rows, block.shape[-1]).astype(BF16)
        return block.reshape(group_rows, block.shape[-1])

    def arrive(j, crosses):
        dispatch(j, crosses).wait_recv()
        spread(j, crosses)

    def relay(crosses):
        @pl.loop(near if crosses else 0, experts if crosses else near)
        def _(j):
            @pl.loop(1, chips)
            def _(k):
                to_far(j, k, crosses).wait_recv()
                to_side(j, k, crosses).start()

    def settle(crosses):
        @pl.loop(near if crosses else 0, experts if crosses else near)
        def _(j):
            @pl.loop(0, chips)
            def _(k):
                to_side(j, k, crosses).wait_recv()

    def group(crosses):
        mine = lax.div(me, near)
        return (1 - mine) if crosses else mine

    def members(crosses):
        return pl.ds(group(crosses) * near, near)

    def hidden_of(crosses):
        g = group(crosses)
        n = 1 if crosses else 0
        return gather(
            lambda b: hidden.at[b, g], lambda k: hid_send.at[n, k], lambda k: hid_recv.at[n, k]
        )

    def up_and_gate(crosses):
        blocks = [join(arrived[p, members(crosses)]) for p in range(parts)]
        for i in range(steps):
            span = slice(i * tile, (i + 1) * tile)

            def product(weights):
                total = None
                for p in range(parts):
                    term = jnp.dot(
                        blocks[p],
                        weights[p * part_width : (p + 1) * part_width, span],
                        preferred_element_type=F32,
                    )
                    total = term if total is None else total + term
                return total

            hidden[tp, group(crosses), :, span] = (
                jax.nn.silu(product(wgate)) * product(wup)
            ).astype(BF16)

    @pl.loop(1, near)
    def _(j):
        arrive(j, False)

    relay(False)
    arrive(near, True)
    keep.wait()
    loads[3].wait()
    loads[4].wait()
    settle(False)
    up_and_gate(False)
    near_across, near_beside, near_begin = hidden_of(False)
    near_begin()

    left = [0] + list(range(max(early, 1), chunks))
    late = experts - near - 1
    if late <= len(left):
        for n in range(late):
            arrive(near + 1 + n, True)
            for i in left[n * len(left) // late : (n + 1) * len(left) // late]:
                convolve(i)
    else:

        @pl.loop(near + 1, experts)
        def _(j):
            arrive(j, True)

        for i in left:
            convolve(i)

    relay(True)
    settle(True)
    up_and_gate(True)
    cross_across, cross_beside, cross_begin = hidden_of(True)
    cross_begin()
    conv_begin()

    loads[6].wait()
    wide = down_sum.shape[1]
    tile, steps = tiles(wide, 256)

    def give_back(j, crosses):
        to = partner(j, 1, crosses)
        return remote(result.at[to], returned.at[me], ret_send.at[j], ret_recv.at[j], ep=to)

    def down(block, crosses, begin):
        deep = pl.ds(pl.multiple_of(block * units, units), units)

        @pl.loop(0, steps)
        def _(i):
            span = pl.ds(pl.multiple_of(i * tile, tile), tile)
            product = jnp.dot(
                hidden[block, group(crosses)], wdown[deep, span], preferred_element_type=F32
            )
            down_sum[:, span] = product if begin else down_sum[:, span] + product

    for crosses, across, beside in (
        (False, near_across, near_beside),
        (True, cross_across, cross_beside),
    ):

        @pl.loop(1, chips)
        def _(k):
            across(k).wait_recv()
            beside(k).start()

        down(tp, crosses, True)
        beside(0).wait_recv()
        down(sibling, crosses, False)

        @pl.loop(1, chips)
        def _(k):
            down(chip_behind(k), crosses, False)
            beside(k).wait_recv()
            down(chip_behind(k) + other - core, crosses, False)

        result[members(crosses)] = down_sum[...].reshape(near, slots, wide).astype(BF16)

        @pl.loop(near if crosses else 1, experts if crosses else near)
        def _(j):
            give_back(j, crosses).start()

        if not crosses:
            own = pltpu.make_async_copy(result.at[me], returned.at[me], self_sem.at[1])
            own.start()

    @pl.loop(1, chips)
    def _(k):
        conv_across(k).wait_recv()
        conv_beside(k).start()

    @pl.loop(0, chips)
    def _(k):
        conv_beside(k).wait_recv()

    width = parts * channels
    chunk, chunks = tiles(length, 64)

    @pl.loop(0, chunks)
    def _(i):
        span = pl.ds(pl.multiple_of(i * chunk, chunk), chunk)
        blocks = [conv[b, span, :].astype(F32) for b in range(parts)]
        center = sum(jnp.sum(block, axis=1, keepdims=True) for block in blocks) / width
        blocks = [block - center for block in blocks]
        spread = sum(jnp.sum(block * block, axis=1, keepdims=True) for block in blocks) / width
        scale = lax.rsqrt(spread + 1e-05)
        for b in range(parts):
            lanes = slice(b * channels, (b + 1) * channels)
            normed = blocks[b] * scale * gain_ref[:, lanes] + shift_ref[:, lanes]
            swished[b, span, :] = jax.nn.silu(normed).astype(BF16)

    loads[5].wait()
    tile, steps = tiles(mixer.shape[1], 256)

    @pl.loop(0, steps)
    def _(i):
        span = pl.ds(pl.multiple_of(i * tile, tile), tile)
        total = jnp.zeros((length, tile), F32)
        for b in range(parts):
            total = total + jnp.dot(
                swished[b], wout[b * channels : (b + 1) * channels, span], preferred_element_type=F32
            )
        mixer[:, span] = total.astype(BF16)

    put_mixer = pltpu.make_async_copy(mixer, mixer_hbm, out_sem.at[0])
    put_mixer.start()

    share = jax.nn.sigmoid(logits_ref[0:1, :] - logits_ref[1:2, :])
    weight = jnp.where(is_first, share * prob_ref[...], 0.0) + jnp.where(
        is_second, (1.0 - share) * prob_ref[...], 0.0
    )
    weights = jnp.where(
        place3, jnp.broadcast_to(weight[:, None, :], (experts, slots, count)), 0.0
    ).reshape(rows, count)
    weights = jnp.transpose(weights, (1, 0))
    high = weights.astype(BF16)
    rest = weights - high.astype(F32)
    middle = rest.astype(BF16)
    low = (rest - middle.astype(F32)).astype(BF16)

    own.wait()

    for crosses in (False, True):

        @pl.loop(near if crosses else 1, experts if crosses else near)
        def _(j):
            give_back(j, crosses).wait_recv()

    tile, steps = tiles(wide, 512)
    for i in range(steps):
        span = slice(i * tile, (i + 1) * tile)
        block = returned[:, :, span]
        if slots % 16:
            block = block.astype(F32).reshape(rows, tile).astype(BF16)
        else:
            block = block.reshape(rows, tile)
        total = jnp.dot(low, block, preferred_element_type=F32)
        total = total + jnp.dot(middle, block, preferred_element_type=F32)
        total = total + jnp.dot(high, block, preferred_element_type=F32)
        combined[:, span] = total.astype(BF16)

    put_expert = pltpu.make_async_copy(combined, expert_hbm, out_sem.at[1])
    put_expert.start()

    for crosses in (False, True):

        @pl.loop(near if crosses else 1, experts if crosses else near)
        def _(j):
            dispatch(j, crosses).wait_send()
            give_back(j, crosses).wait_send()

        @pl.loop(near if crosses else 0, experts if crosses else near)
        def _(j):
            @pl.loop(1, chips)
            def _(k):
                to_far(j, k, crosses).wait_send()

            @pl.loop(0, chips)
            def _(k):
                to_side(j, k, crosses).wait_send()

    for across, beside in (
        (conv_across, conv_beside),
        (near_across, near_beside),
        (cross_across, cross_beside),
    ):

        @pl.loop(1, chips)
        def _(k):
            across(k).wait_send()

        @pl.loop(0, chips)
        def _(k):
            beside(k).wait_send()

    put_mixer.wait()
    put_expert.wait()


def local(
    experts,
    parts,
    conv_value,
    conv_gate,
    conv_kernel,
    norm_gain,
    norm_shift,
    out_weight,
    expert_input,
    expert_ids,
    pair_logits,
    group_prob,
    expert_gate,
    expert_up,
    expert_down,
):
    channels, length = conv_value.shape
    count, model = expert_input.shape
    slots = 2 * count // experts
    rows = experts * slots
    part_width = model // parts
    units, wide = expert_gate.shape[2], expert_down.shape[2]
    out_width = out_weight.shape[1]
    chips = parts // CORES
    edge = -(-((conv_kernel.shape[0] - 1) // 2) // 16) * 16
    anywhere = pl.BlockSpec(memory_space=pl.ANY)
    near = pl.BlockSpec(memory_space=pltpu.VMEM)
    dma = pltpu.SemaphoreType.DMA
    return pl.pallas_call(
        functools.partial(kernel, experts, parts),
        out_shape=(
            jax.ShapeDtypeStruct((length, out_width), BF16),
            jax.ShapeDtypeStruct((count, wide), BF16),
        ),
        in_specs=[anywhere] * 7 + [near] * 6,
        out_specs=(anywhere, anywhere),
        scratch_shapes=[
            pltpu.VMEM((channels, length), BF16),
            pltpu.VMEM((channels, length), BF16),
            pltpu.VMEM((count, part_width), BF16),
            pltpu.VMEM((model, units), BF16),
            pltpu.VMEM((model, units), BF16),
            pltpu.VMEM(expert_down.shape[1:], BF16),
            pltpu.VMEM(out_weight.shape, BF16),
            pltpu.VMEM((experts, slots, part_width), BF16),
            pltpu.VMEM((parts, experts, slots, part_width), BF16),
            pltpu.VMEM((parts, 2, rows // 2, units), BF16),
            pltpu.VMEM((rows // 2, wide), F32),
            pltpu.VMEM((experts, slots, wide), BF16),
            pltpu.VMEM((experts, slots, wide), BF16),
            pltpu.VMEM((length + 2 * edge, channels), F32),
            pltpu.VMEM((2, edge, channels), BF16),
            pltpu.VMEM((2, edge, channels), BF16),
            pltpu.VMEM((parts, length, channels), BF16),
            pltpu.VMEM((parts, length, channels), BF16),
            pltpu.VMEM((length, out_width), BF16),
            pltpu.VMEM((count, wide), BF16),
            dma((7,)),
            dma((2,)),
            dma((2,)),
            dma((experts,)),
            dma((experts,)),
            dma((chips * experts,)),
            dma((chips * experts,)),
            dma((chips * experts,)),
            dma((chips * experts,)),
            dma((2,)),
            dma((2,)),
            dma((2 * chips,)),
            dma((2 * chips,)),
            dma((2, 2 * chips)),
            dma((2, 2 * chips)),
            dma((experts,)),
            dma((experts,)),
        ],
        compiler_params=pltpu.CompilerParams(
            collective_id=0, has_side_effects=True, vmem_limit_bytes=60 * 1024 * 1024
        ),
        name="block",
    )(
        conv_value,
        conv_gate,
        expert_input,
        expert_gate,
        expert_up,
        expert_down,
        out_weight,
        conv_kernel,
        norm_gain[None, :],
        norm_shift[None, :],
        expert_ids.T,
        pair_logits.T,
        group_prob[None, :],
    )


def solution(mesh):
    placed = (
        P("tp", "ep"),
        P("tp", "ep"),
        P(None, "tp"),
        P(),
        P(),
        P(None, "tp"),
        P("ep", None),
        P("ep", None),
        P("ep", None),
        P("ep"),
        P("ep", None, "tp"),
        P("ep", None, "tp"),
        P("ep", None, "tp"),
    )
    return jax.shard_map(
        functools.partial(local, mesh.shape["ep"], mesh.shape["tp"]),
        mesh=mesh,
        in_specs=placed,
        out_specs=(P("ep", "tp"), P("ep", "tp")),
        check_vma=False,
    )
```
